128 devices in a mesh: ep: 32 (over z, y, core), tp: 4 (over x).
Axes of the slice: x: 4, y: 4, z: 4, core: 2. Of those that a mesh axis runs over, the one named last changes fastest.
Arguments:
- q_latent: bfloat16 [16384, 512], P(('ep', 'tp')), may hold values from -6 to 6
- kv_latent: bfloat16 [16384, 256], P(('ep', 'tp')), may hold values from -6 to 6
- rope_key: bfloat16 [16384, 32], P(('ep', 'tp')), may hold values from -240 to 240
- q_gain: float32 [512], replicated, may hold values from 0.1 to 1.9
- kv_gain: float32 [256], replicated, may hold values from 0.1 to 1.9
- w_query: bfloat16 [512, 1024], P(None, 'tp'), may hold values from -0.25 to 0.25
- w_query_rot: bfloat16 [512, 512], P(None, 'tp'), may hold values from -0.25 to 0.25
- w_key: bfloat16 [256, 1024], P(None, 'tp'), may hold values from -0.375 to 0.375
- w_value: bfloat16 [256, 1024], P(None, 'tp'), may hold values from -0.375 to 0.375
- w_mix_out: bfloat16 [1024, 2048], P('tp'), may hold values from -0.1875 to 0.1875
- expert_input: bfloat16 [16384, 2048], P(('ep', 'tp')), may hold values from -6 to 6
- ffn_gain: float32 [2048], replicated, may hold values from 0.1 to 1.9
- expert_ids: int32 [16384, 4], P(('ep', 'tp')), may hold values from 0 to 31, all different within a row; in each aligned block of 128 rows (0 to 127, 128 to 255, ...) at most 24 rows name the same one
- route_weights: float32 [16384, 4], P(('ep', 'tp')), may hold values from 0.2 to 1
- w_gate_exp: bfloat16 [32, 2048, 1024], P('ep', None, 'tp'), may hold values from -0.125 to 0.125
- w_up_exp: bfloat16 [32, 2048, 1024], P('ep', None, 'tp'), may hold values from -0.125 to 0.125
- w_down_exp: bfloat16 [32, 1024, 2048], P('ep', 'tp'), may hold values from -0.1875 to 0.1875
Outputs:
- mixer_out: bfloat16 [16384, 2048], P(('ep', 'tp'))
- expert_out: bfloat16 [16384, 2048], P(('ep', 'tp'))
The draws below stay inside these ranges and needn't reach their ends.
Inputs may be any that keep to these rules, and one draw needn't show every extreme that they name: `expert_ids`: the experts of a row are all different. In the rows of one device (aligned blocks of 128 tokens) no expert is named by more than 24 rows, a bound that some block reaches.
All inputs are finite; a program needn't handle non-finite values.
Results may differ from the reference program's by a relative error of at most 0.012.
The reference program's roundings to bfloat16 on the way count: a program that leaves them out, or rounds other values in their place, can miss the bound.
Values may be sent and summed in bfloat16 or wider, within the bound.
A program may use at most 128 MiB of HBM per device.

```python
import math
import jax
import jax.numpy as jnp
import numpy as np
from jax import lax

D = 2048
HEADS = 16
NOPE = 64
ROPE = 32
VD = 64
Q_RANK = 512
KV_RANK = 256
FF = 1024
TOPK = 4
SEG = 64
TOK_DEV = 128
EXPERTS = 32
TOKENS = 16384
CAP = 24
N_EP = 32
N_TP = 4


def draw_rope_key(key, part):
    drawn = jnp.clip(jax.random.normal(jax.random.fold_in(key, 11), (TOKENS, ROPE), jnp.float32), -6.0, 6.0)
    return drawn.astype(jnp.bfloat16)


def levels(key, dims, split, least, high):
    loudness = 1.0
    for position, blocks in split:
        steps = jax.random.uniform(jax.random.fold_in(jax.random.fold_in(key, 6), position), (blocks,), jnp.float32, least / len(split), high / len(split))
        loudness = loudness * jnp.repeat(jnp.exp(steps), dims[position] // blocks).reshape((-1,) + (1,) * (len(dims) - 1 - position))
    return loudness


def deal_out(key, own, number, rows, number_of, top, bound, skew):
    order = jax.random.permutation(key, number_of)
    packed, ordinary = shares(number_of, rows * top, bound, skew, True), shares(number_of, rows * top, bound, skew, False)
    places = jnp.arange(number_of)

    def named(tallies, offset_by):
        used = int((tallies > 0).sum())
        fixed = max(1, used // 4)
        moved = fixed + (places - fixed + offset_by * (used - fixed)) % max(1, number_of - fixed)
        return jnp.zeros((number_of,), jnp.int32).at[order[jnp.where(places < fixed, places, moved)]].set(jnp.asarray(tallies, jnp.int32))

    tallies = jnp.where(number % 4 == 0, named(packed, number // 4), named(ordinary, number - number // 4 - 1))
    mixed = jax.random.permutation(jax.random.fold_in(own, 3), number_of)
    giver, taker = mixed[0:number_of // 2 * 2:2], mixed[1:number_of // 2 * 2:2]
    slack = jnp.minimum(tallies[giver] - 1, bound - tallies[taker]) // 2
    slack = jnp.where((giver == order[0]) | (taker == order[0]) | (tallies[taker] == 0), 0, jnp.maximum(slack, 0))
    moved = jax.random.randint(jax.random.fold_in(own, 4), (number_of // 2,), 0, 1 << 20) % (slack + 1)
    tallies = tallies.at[giver].add(-moved).at[taker].add(moved)
    members = jnp.searchsorted(jnp.cumsum(tallies), jnp.arange(rows * top), side="right").astype(jnp.int32)
    grid = members.reshape(top, rows).T
    grid = grid[jax.random.permutation(jax.random.fold_in(own, 1), rows)]
    offset_by = jax.random.randint(jax.random.fold_in(own, 2), (rows, 1), 0, top)
    return jnp.take_along_axis(grid, (jnp.arange(top)[None, :] + offset_by) % top, axis=1)


def shares(amount, total, limit, lean, full):
    weights = [(1 << 20) // math.isqrt(rank ** lean) + 1 for rank in range(1, amount + 1)]
    largest = limit if full else min(limit, max(-(-total // amount), total * weights[0] // sum(weights)))
    least = 1 if total - largest >= amount - 1 else 0
    holding, surplus = [largest] + [least] * (amount - 1), total - largest - least * (amount - 1)
    while surplus > 0:
        free = [i for i in range(1, amount) if holding[i] < largest] or [i for i in range(1, amount) if holding[i] < limit]
        whole, budget = sum([weights[i] for i in free]), surplus
        for i in free:
            more = min(limit - holding[i], max(1, budget * weights[i] // whole), surplus)
            holding[i] = holding[i] + more
            surplus = surplus - more
    return np.array(holding)


def noise(key, dims, width, limit, split=(), kind=jnp.bfloat16):
    result = width * jax.random.normal(key, dims, jnp.float32)
    if split:
        result = result * levels(key, dims, split, -0.22, 0.18)
    return jnp.clip(result, -limit, limit).astype(kind)


def setup_inputs(seed: int = 0) -> dict:
    keys = jax.random.split(jax.random.key(seed), 18)
    q_latent = noise(keys[0], (TOKENS, Q_RANK), 1.0, 6.0, ((0, 128),))
    kv_latent = noise(keys[1], (TOKENS, KV_RANK), 1.0, 6.0, ((0, 128),))
    rope_key = draw_rope_key(jax.random.fold_in(keys[17], 71), 0)
    q_gain = jnp.clip(1.0 + 0.18 * jax.random.normal(keys[3], (Q_RANK,), jnp.float32), 0.1, 1.9)
    kv_gain = jnp.clip(1.0 + 0.18 * jax.random.normal(keys[4], (KV_RANK,), jnp.float32), 0.1, 1.9)
    w_query = noise(keys[5], (Q_RANK, HEADS * NOPE), Q_RANK ** -0.5, 0.25, ((1, 4),))
    w_query_rot = noise(keys[6], (Q_RANK, HEADS * ROPE), Q_RANK ** -0.5, 0.25, ((1, 4),))
    w_key = noise(keys[7], (KV_RANK, HEADS * NOPE), KV_RANK ** -0.5, 0.375, ((1, 4),))
    w_value = noise(keys[8], (KV_RANK, HEADS * VD), KV_RANK ** -0.5, 0.375, ((1, 4),))
    w_mix_out = noise(keys[9], (HEADS * VD, D), (HEADS * VD) ** -0.5, 0.1875, ((0, 4),))
    expert_input = noise(keys[10], (TOKENS, D), 1.0, 6.0, ((0, 128),))
    ffn_gain = jnp.clip(1.0 + 0.18 * jax.random.normal(keys[11], (D,), jnp.float32), 0.1, 1.9)
    expert_ids_keys = jax.random.split(jax.random.fold_in(keys[12], 1), TOKENS // TOK_DEV)
    expert_ids_turns = jax.random.permutation(jax.random.fold_in(keys[12], 3), TOKENS // TOK_DEV)
    expert_ids = jax.vmap(lambda own, number: deal_out(jax.random.fold_in(keys[12], 2), own, number, TOK_DEV, EXPERTS, TOPK, CAP, 2))(expert_ids_keys, expert_ids_turns).reshape((TOKENS, TOPK))
    route_weights = jnp.clip(0.2 + 0.8 * jax.random.uniform(keys[13], (TOKENS, TOPK), jnp.float32) ** levels(keys[13], (TOKENS, TOPK), ((0, 128),), -0.2, 0.2), 0.2, 1.0)
    w_gate_exp = noise(keys[14], (EXPERTS, D, FF), D ** -0.5, 0.125, ((0, 32), (2, 4)))
    w_up_exp = noise(keys[15], (EXPERTS, D, FF), D ** -0.5, 0.125, ((0, 32), (2, 4)))
    w_down_exp = noise(keys[16], (EXPERTS, FF, D), FF ** -0.5, 0.1875, ((0, 32), (1, 4)))
    return dict(q_latent=q_latent, kv_latent=kv_latent, rope_key=rope_key, q_gain=q_gain, kv_gain=kv_gain, w_query=w_query, w_query_rot=w_query_rot, w_key=w_key, w_value=w_value, w_mix_out=w_mix_out, expert_input=expert_input, ffn_gain=ffn_gain, expert_ids=expert_ids, route_weights=route_weights, w_gate_exp=w_gate_exp, w_up_exp=w_up_exp, w_down_exp=w_down_exp)


norm_epsilon = 1e-06
rope_base = 10000.0
query_block = 256

def rms_scale(values_in, gain_vec):
    floats = values_in.astype(jnp.float32)
    return floats * lax.rsqrt(lax.optimization_barrier(jnp.mean(floats * floats, axis=-1, keepdims=True)) + norm_epsilon) * gain_vec

def tables(positions):
    half_width = ROPE // 2
    frequency = rope_base ** (-jnp.arange(half_width, dtype=jnp.float32) / half_width)
    angles = positions.astype(jnp.float32)[:, None] * frequency[None, :]
    return (jnp.cos(angles), jnp.sin(angles))

def rotate_pairs(values_in, cosine, sine_table):
    half_width = values_in.shape[-1] // 2
    first, second = (values_in[..., :half_width], values_in[..., half_width:])
    return jnp.concatenate([first * cosine - second * sine_table, first * sine_table + second * cosine], axis=-1)

def mixer(q_latent, kv_latent, rope_key, q_gain, kv_gain, w_query, w_query_rot, w_key, w_value, w_mix_out):
    row_total = q_latent.shape[0]
    positions = jnp.arange(row_total, dtype=jnp.int32)
    cosine, sine_table = tables(positions)
    q_normed = rms_scale(q_latent, q_gain).astype(jnp.bfloat16)
    q_plain = jnp.dot(q_normed, w_query, preferred_element_type=jnp.float32).astype(jnp.bfloat16)
    q_plain = q_plain.reshape(row_total, HEADS, NOPE)
    q_turned = jnp.dot(q_normed, w_query_rot, preferred_element_type=jnp.float32).reshape(row_total, HEADS, ROPE)
    q_turned = rotate_pairs(q_turned, cosine[:, None, :], sine_table[:, None, :]).astype(jnp.bfloat16)
    kv_normed = rms_scale(kv_latent, kv_gain).astype(jnp.bfloat16)
    k_plain = jnp.dot(kv_normed, w_key, preferred_element_type=jnp.float32).astype(jnp.bfloat16)
    k_plain = k_plain.reshape(row_total, HEADS, NOPE).astype(jnp.float32)
    values = jnp.dot(kv_normed, w_value, preferred_element_type=jnp.float32).astype(jnp.bfloat16)
    values = values.reshape(row_total, HEADS, VD).astype(jnp.float32)
    k_turned = rotate_pairs(rope_key.astype(jnp.float32), cosine, sine_table).astype(jnp.bfloat16).astype(jnp.float32)
    segment = positions // SEG
    score_scale = (NOPE + ROPE) ** (-0.5)

    def attend(first_row):
        block_plain = lax.dynamic_slice_in_dim(q_plain, first_row, query_block, 0).astype(jnp.float32)
        block_turned = lax.dynamic_slice_in_dim(q_turned, first_row, query_block, 0).astype(jnp.float32)
        scores = jnp.einsum('qhd,khd->hqk', block_plain, k_plain) + jnp.einsum('qhd,kd->hqk', block_turned, k_turned)
        scores = scores * score_scale
        query_segment = (first_row + jnp.arange(query_block, dtype=jnp.int32)) // SEG
        allowed = segment[None, :] <= query_segment[:, None]
        scores = jnp.where(allowed[None], scores, -jnp.inf)
        row_max = lax.optimization_barrier(jnp.max(scores, axis=-1, keepdims=True))
        weights = jnp.where(allowed[None], jnp.exp(scores - row_max), 0.0)
        weight_sum = lax.optimization_barrier(jnp.sum(weights, axis=-1))
        rounded = weights.astype(jnp.bfloat16).astype(jnp.float32)
        mixed = jnp.einsum('hqk,khd->qhd', rounded, values) / jnp.transpose(weight_sum)[:, :, None]
        return mixed.astype(jnp.bfloat16).reshape(query_block, HEADS * VD)
    starts = jnp.arange(0, row_total, query_block, dtype=jnp.int32)
    attention = lax.map(attend, starts).reshape(row_total, HEADS * VD)
    block_width = HEADS * VD // N_TP
    summed = jnp.zeros((row_total, D), jnp.float32)
    for block_index in range(N_TP):
        columns = attention[:, block_index * block_width:(block_index + 1) * block_width]
        weight_rows = w_mix_out[block_index * block_width:(block_index + 1) * block_width]
        partial_out = jnp.dot(columns, weight_rows, preferred_element_type=jnp.float32).astype(jnp.bfloat16)
        summed = summed + lax.optimization_barrier(partial_out).astype(jnp.float32)
    return summed.astype(jnp.bfloat16)

def experts(expert_input, ffn_gain, expert_ids, route_weights, w_gate_exp, w_up_exp, w_down_exp):
    row_total = expert_input.shape[0]
    groups = N_EP * N_TP
    expert_count = w_gate_exp.shape[0]
    normed = rms_scale(expert_input, ffn_gain).astype(jnp.bfloat16)
    routed = expert_ids.reshape(groups, TOK_DEV * TOPK).astype(jnp.int32)
    onehot = (routed[:, :, None] == jnp.arange(expert_count, dtype=jnp.int32)[None, None, :]).astype(jnp.int32)
    slot_number = lax.optimization_barrier(jnp.sum((jnp.cumsum(onehot, axis=1) - 1) * onehot, axis=-1)).astype(jnp.int32)
    group_index = jnp.arange(groups, dtype=jnp.int32)[:, None]
    slot_place = ((routed * groups + group_index) * CAP + slot_number).reshape(-1).astype(jnp.int32)
    token_index = group_index * TOK_DEV + jnp.arange(TOK_DEV * TOPK, dtype=jnp.int32)[None, :] // TOPK
    token_table = jnp.zeros((expert_count * groups * CAP,), jnp.int32).at[slot_place].set(token_index.reshape(-1).astype(jnp.int32))
    token_table = token_table.reshape(expert_count, groups * CAP)
    block_width = FF // N_TP

    def expert_block(arguments):
        rows_idx, gate_weight, up_weight, down_weight = arguments
        chosen = normed[rows_idx]
        gate_part = jnp.dot(chosen, gate_weight, preferred_element_type=jnp.float32)
        up_part = jnp.dot(chosen, up_weight, preferred_element_type=jnp.float32)
        hidden = (jax.nn.silu(gate_part) * up_part).astype(jnp.bfloat16)
        summed = jnp.zeros((chosen.shape[0], D), jnp.float32)
        for block_index in range(N_TP):
            columns = hidden[:, block_index * block_width:(block_index + 1) * block_width]
            weight_rows = down_weight[block_index * block_width:(block_index + 1) * block_width]
            partial_out = jnp.dot(columns, weight_rows, preferred_element_type=jnp.float32).astype(jnp.bfloat16)
            summed = summed + lax.optimization_barrier(partial_out).astype(jnp.float32)
        return summed.astype(jnp.bfloat16)
    results = lax.map(expert_block, (token_table, w_gate_exp, w_up_exp, w_down_exp))
    all_results = results.reshape(-1, D)
    picked = all_results[slot_place].astype(jnp.float32).reshape(row_total, TOPK, D)
    weighted_sum = lax.optimization_barrier(jnp.sum(picked * route_weights[:, :, None].astype(jnp.float32), axis=1))
    return weighted_sum.astype(jnp.bfloat16)

def reference(q_latent, kv_latent, rope_key, q_gain, kv_gain, w_query, w_query_rot, w_key, w_value, w_mix_out, expert_input, ffn_gain, expert_ids, route_weights, w_gate_exp, w_up_exp, w_down_exp):
    mixer_out = mixer(q_latent, kv_latent, rope_key, q_gain, kv_gain, w_query, w_query_rot, w_key, w_value, w_mix_out)
    expert_out = experts(expert_input, ffn_gain, expert_ids, route_weights, w_gate_exp, w_up_exp, w_down_exp)
    return (mixer_out, expert_out)
```

```python
import functools
import math
import jax
import jax.numpy as jnp
from jax import lax
from jax.experimental import pallas as pl
from jax.experimental.pallas import tpu as pltpu
from jax.sharding import PartitionSpec as P

D = 2048
NOPE = 64
ROPE = 32
VD = 64
TOPK = 4
SEG = 64
LOW = -1e30

norm_epsilon = 1e-06
rope_base = 10000.0
bf16 = jnp.bfloat16
f32 = jnp.float32


def rms_scale(values_in, gain_vec):
    floats = values_in.astype(f32)
    return (
        floats
        * lax.rsqrt(jnp.mean(floats * floats, axis=-1, keepdims=True) + norm_epsilon)
        * gain_vec
    )


def tables(positions):
    half_width = ROPE // 2
    frequency = rope_base ** (-jnp.arange(half_width, dtype=f32) / half_width)
    angles = positions.astype(f32)[:, None] * frequency[None, :]
    return (jnp.cos(angles), jnp.sin(angles))


def rotate_pairs(values_in, cosine, sine_table):
    half_width = values_in.shape[-1] // 2
    first, second = (values_in[..., :half_width], values_in[..., half_width:])
    return jnp.concatenate(
        [first * cosine - second * sine_table, first * sine_table + second * cosine], axis=-1
    )


def attention_kernel(idx_ref, q_ref, kv_ref, wk_ref, wv_ref, out_ref, top, acc, *, heads, rows, coef):
    step = pl.program_id(0)
    last = idx_ref[0]

    @pl.when(step == 0)
    def _():
        top[...] = jnp.full(top.shape, LOW, f32)
        acc[...] = jnp.zeros(acc.shape, f32)

    def block(masked):
        piece = kv_ref[0]
        count = piece.shape[0]
        latent = piece.shape[2]
        normed = piece[:, :rows, :].reshape(count * rows, latent)
        tails = [piece[t, rows:, :] for t in range(count)]
        first = jnp.concatenate([u[:, :rows] for u in tails], axis=1)
        second = jnp.concatenate([u[:, rows:] for u in tails], axis=1)
        turned = jnp.concatenate([first, second], axis=0)
        keys = lax.dot_general(
            wk_ref[...], normed, (((1,), (1,)), ((), ())), preferred_element_type=f32
        ).astype(bf16)
        vals = jnp.dot(normed, wv_ref[...], preferred_element_type=f32)
        lane = lax.broadcasted_iota(jnp.int32, vals.shape, 1) % 128
        vals = jnp.where(lane >= VD, 1.0, vals).astype(bf16)
        for h in range(heads):
            key_cols = jnp.concatenate([keys[h * NOPE : (h + 1) * NOPE], turned], axis=0)
            s = jnp.dot(q_ref[h], key_cols, preferred_element_type=f32)
            if masked:
                query_seg = lax.broadcasted_iota(jnp.int32, s.shape, 0) // SEG
                key_seg = lax.broadcasted_iota(jnp.int32, s.shape, 1) // SEG
                s = jnp.where(key_seg <= query_seg, s, LOW)
            old = top[h]
            new = jnp.maximum(old, jnp.max(s, axis=1, keepdims=True))
            p = jnp.exp2((s - new[:, :1]) * coef).astype(bf16)
            factor = jnp.exp2((old - new) * coef)
            acc[h] = acc[h] * factor + jnp.dot(
                p, vals[:, h * 128 : (h + 1) * 128], preferred_element_type=f32
            )
            top[h] = new

    @pl.when(step < last)
    def _():
        block(False)

    @pl.when(step == last)
    def _():
        block(True)
        for pair in range(heads // 2):
            parts = []
            for h in (2 * pair, 2 * pair + 1):
                a = acc[h]
                parts.append(a[:, :VD] / a[:, VD:])
            out_ref[:, pair * 128 : (pair + 1) * 128] = jnp.concatenate(parts, axis=1).astype(bf16)


def attend(group, q_cat, kv, wk_turned, wv_wide):
    heads, queries, depth = q_cat.shape
    blocks, count, piece_rows, latent = kv.shape
    rows = queries // count
    coef = ((NOPE + ROPE) ** -0.5) * math.log2(math.e)
    return pl.pallas_call(
        functools.partial(attention_kernel, heads=heads, rows=rows, coef=coef),
        out_shape=jax.ShapeDtypeStruct((queries, heads * VD), bf16),
        grid_spec=pltpu.PrefetchScalarGridSpec(
            num_scalar_prefetch=1,
            grid=(blocks,),
            in_specs=[
                pl.BlockSpec((heads, queries, depth), lambda i, n: (0, 0, 0)),
                pl.BlockSpec(
                    (1, count, piece_rows, latent), lambda i, n: (jnp.minimum(i, n[0]), 0, 0, 0)
                ),
                pl.BlockSpec(wk_turned.shape, lambda i, n: (0, 0)),
                pl.BlockSpec(wv_wide.shape, lambda i, n: (0, 0)),
            ],
            out_specs=pl.BlockSpec((queries, heads * VD), lambda i, n: (0, 0)),
            scratch_shapes=[
                pltpu.VMEM((heads, queries, 128), f32),
                pltpu.VMEM((heads, queries, 128), f32),
            ],
        ),
        compiler_params=pltpu.CompilerParams(
            dimension_semantics=("arbitrary",), vmem_limit_bytes=32 << 20
        ),
        cost_estimate=pl.CostEstimate(
            flops=12 * 10**9, transcendentals=34 * 10**6, bytes_accessed=10**7
        ),
    )(group, q_cat, kv, wk_turned, wv_wide)


def on_device(
    q_latent,
    kv_latent,
    rope_key,
    q_gain,
    kv_gain,
    w_query,
    w_query_rot,
    w_key,
    w_value,
    w_mix_out,
    expert_input,
    ffn_gain,
    expert_ids,
    route_weights,
    w_gate_exp,
    w_up_exp,
    w_down_exp,
):
    tok_rows = q_latent.shape[0]
    tp_count = lax.axis_size("tp")
    expert_count = lax.axis_size("ep")
    group = lax.axis_index("ep")
    place = lax.axis_index("tp")
    group_rows = tp_count * tok_rows
    heads_here = w_key.shape[1] // NOPE
    latent_width = kv_latent.shape[1]

    slot_count = 3 * tok_rows * TOPK // (2 * expert_count)
    normed = rms_scale(expert_input, ffn_gain).astype(bf16)
    routed = expert_ids.reshape(-1)
    onehot = (routed[:, None] == jnp.arange(expert_count, dtype=jnp.int32)[None, :]).astype(
        jnp.int32
    )
    slot_number = jnp.sum((jnp.cumsum(onehot, axis=0) - 1) * onehot, axis=-1)
    slot_place = (routed * slot_count + slot_number).reshape(tok_rows, TOPK)
    slot_line = jnp.arange(expert_count * slot_count, dtype=jnp.int32)
    picks = [
        (slot_place[:, rank][:, None] == slot_line[None, :]).astype(bf16) for rank in range(TOPK)
    ]
    dispatch = picks[0]
    for rank in range(1, TOPK):
        dispatch = dispatch + picks[rank]
    outgoing = lax.dot_general(
        dispatch, normed, (((0,), (0,)), ((), ())), preferred_element_type=f32
    ).astype(bf16)
    arrived = lax.all_to_all(
        outgoing.reshape(expert_count, slot_count, D), "ep", split_axis=0, concat_axis=0, tiled=True
    )

    token_start = group * group_rows + place * tok_rows
    cosine, sine_table = tables(token_start + jnp.arange(tok_rows, dtype=jnp.int32))
    kv_normed = rms_scale(kv_latent, kv_gain).astype(bf16)
    k_turned = rotate_pairs(rope_key.astype(f32), cosine, sine_table).astype(bf16)
    half_width = ROPE // 2
    tail = jnp.concatenate([k_turned[:, :half_width].T, k_turned[:, half_width:].T], axis=1)
    piece = jnp.concatenate([kv_normed, tail], axis=0)
    pieces = lax.all_gather(piece, ("ep", "tp"), axis=0, tiled=True)
    kv = pieces.reshape(expert_count, tp_count, tok_rows + half_width, latent_width)

    right = [(i, (i + 1) % tp_count) for i in range(tp_count)]
    left = [(i, (i - 1) % tp_count) for i in range(tp_count)]
    own = (w_gate_exp[0], w_up_exp[0], w_down_exp[0])
    from_left = [lax.ppermute(w, "tp", right) for w in own]
    from_right = [lax.ppermute(w, "tp", left) for w in own]

    q_rows = lax.all_gather(rms_scale(q_latent, q_gain).astype(bf16), "tp", axis=0, tiled=True)
    cosine, sine_table = tables(group * group_rows + jnp.arange(group_rows, dtype=jnp.int32))
    plain = jnp.dot(q_rows, w_query, preferred_element_type=f32).astype(bf16)
    turned = jnp.dot(q_rows, w_query_rot, preferred_element_type=f32).reshape(
        group_rows, heads_here, ROPE
    )
    turned = rotate_pairs(turned, cosine[:, None, :], sine_table[:, None, :]).astype(bf16)
    q_cat = jnp.concatenate(
        [plain.reshape(group_rows, heads_here, NOPE), turned], axis=2
    ).transpose(1, 0, 2)
    wv_wide = jnp.concatenate(
        [
            w_value.reshape(latent_width, heads_here, VD),
            jnp.zeros((latent_width, heads_here, 128 - VD), bf16),
        ],
        axis=2,
    ).reshape(latent_width, heads_here * 128)
    attention = attend(
        group.astype(jnp.int32).reshape(1), q_cat, kv, w_key.T, wv_wide
    )

    def far(array_index, axis):
        a, b = from_left[array_index], from_right[array_index]
        half = a.shape[axis] // 2
        first = lax.ppermute(lax.slice_in_dim(a, 0, half, axis=axis), "tp", right)
        second = lax.ppermute(lax.slice_in_dim(b, half, 2 * half, axis=axis), "tp", left)
        return jnp.concatenate([first, second], axis=axis)

    opposite = [far(0, 0), far(1, 0), far(2, 0)]

    partial_mix = jnp.dot(attention, w_mix_out, preferred_element_type=f32).astype(bf16)
    mix_blocks = lax.all_to_all(
        partial_mix.reshape(tp_count, tok_rows, D), "tp", split_axis=0, concat_axis=0, tiled=True
    )
    mixer_out = jnp.sum(mix_blocks.astype(f32), axis=0).astype(bf16)

    chosen = arrived.reshape(expert_count * slot_count, D)
    summed = None
    for gate_weight, up_weight, down_weight in (own, from_left, from_right, opposite):
        gate_part = jnp.dot(chosen, gate_weight, preferred_element_type=f32)
        up_part = jnp.dot(chosen, up_weight, preferred_element_type=f32)
        hidden = (jax.nn.silu(gate_part) * up_part).astype(bf16)
        block = jnp.dot(hidden, down_weight, preferred_element_type=f32).astype(bf16)
        block = lax.optimization_barrier(block).astype(f32)
        summed = block if summed is None else summed + block
    results = lax.all_to_all(
        summed.astype(bf16).reshape(expert_count, slot_count, D),
        "ep",
        split_axis=0,
        concat_axis=0,
        tiled=True,
    ).reshape(expert_count * slot_count, D)
    combined = jnp.zeros((tok_rows, D), f32)
    for rank in range(TOPK):
        fetched = jnp.dot(picks[rank], results, preferred_element_type=f32)
        combined = combined + route_weights[:, rank : rank + 1] * fetched
    return (mixer_out, combined.astype(bf16))


def solution(mesh):
    return jax.shard_map(
        on_device,
        mesh=mesh,
        in_specs=(
            P(("ep", "tp"), None),
            P(("ep", "tp"), None),
            P(("ep", "tp"), None),
            P(),
            P(),
            P(None, "tp"),
            P(None, "tp"),
            P(None, "tp"),
            P(None, "tp"),
            P("tp", None),
            P(("ep", "tp"), None),
            P(),
            P(("ep", "tp"), None),
            P(("ep", "tp"), None),
            P("ep", None, "tp"),
            P("ep", None, "tp"),
            P("ep", "tp", None),
        ),
        out_specs=(P(("ep", "tp"), None), P(("ep", "tp"), None)),
        check_vma=False,
    )
```

```python
import functools
import math
import jax
import jax.numpy as jnp
from jax import lax
from jax.experimental import pallas as pl
from jax.experimental.pallas import tpu as pltpu
from jax.sharding import PartitionSpec as P

D = 2048
NOPE = 64
ROPE = 32
VD = 64
TOPK = 4
SEG = 64
LOW = -1e30
EP = 32
TP = 4

norm_epsilon = 1e-06
rope_base = 10000.0
bf16 = jnp.bfloat16
f32 = jnp.float32


def rms_scale(values_in, gain_vec):
    floats = values_in.astype(f32)
    return (
        floats
        * lax.rsqrt(jnp.mean(floats * floats, axis=-1, keepdims=True) + norm_epsilon)
        * gain_vec
    )


def tables(positions):
    half_width = ROPE // 2
    frequency = rope_base ** (-jnp.arange(half_width, dtype=f32) / half_width)
    angles = positions.astype(f32)[:, None] * frequency[None, :]
    return (jnp.cos(angles), jnp.sin(angles))


def rotate_pairs(values_in, cosine, sine_table):
    half_width = values_in.shape[-1] // 2
    first, second = (values_in[..., :half_width], values_in[..., half_width:])
    return jnp.concatenate(
        [first * cosine - second * sine_table, first * sine_table + second * cosine], axis=-1
    )


def gather_kernel(
    piece_ref, q_ref, out_ref, q_out, own_sem, send, recv, across_send, across_recv, q_send, q_recv
):
    ep = lax.axis_index("ep")
    me = {"z": ep // 8, "y": (ep // 2) % 4, "x": lax.axis_index("tp")}
    core = ep % 2
    parts = out_ref.shape[4] // 48

    def device(place, side):
        return {"ep": place["z"] * 8 + place["y"] * 2 + side, "tp": place["x"]}

    def moved(axis, offset):
        place = dict(me)
        place[axis] = (me[axis] + offset) % 4
        return place

    def mirrored(offset):
        return {"ep": EP - 1 - ep, "tp": (me["x"] + offset) % 4}

    orders = (("x", "y", "z"), ("y", "z", "x"), ("z", "x", "y"))
    barrier = pltpu.get_barrier_semaphore()
    for axis in "xyz":
        for offset in (1, 2, 3):
            pl.semaphore_signal(barrier, inc=1, device_id=device(moved(axis, offset), core))
    pl.semaphore_signal(barrier, inc=1, device_id=device(me, 1 - core))
    for offset in range(4):
        pl.semaphore_signal(barrier, inc=1, device_id=mirrored(offset))
    pl.semaphore_wait(barrier, 14)

    own = pltpu.make_async_copy(piece_ref, out_ref.at[me["z"], me["y"], core, me["x"]], own_sem)
    own.start()
    side = ep // (EP // 2)
    half = q_ref.shape[0] // 2
    q_own = pltpu.make_async_copy(q_ref.at[pl.ds(0, half)], q_out.at[side, me["x"]], q_send.at[0])
    q_own.start()
    own.wait()

    def q_copy(index, part, place):
        offset = index % 4
        target = mirrored(offset) if index >= 4 else device(moved("x", offset), core)
        return pltpu.make_async_remote_copy(
            src_ref=q_ref.at[pl.ds(half * (index // 4), half)],
            dst_ref=q_out.at[part, place],
            send_sem=q_send.at[index],
            recv_sem=q_recv.at[index],
            device_id=target,
        )

    def region(part, full, place, side):
        at = [slice(None) if axis in full else place[axis] for axis in "zyx"]
        return out_ref.at[at[0], at[1], side, at[2], pl.ds(48 * part, 48), :]

    def hop(part, phase, offset, place):
        axis = orders[part][phase]
        view = region(part, orders[part][:phase], place, core)
        return pltpu.make_async_remote_copy(
            src_ref=view, dst_ref=view,
            send_sem=send.at[part, phase, offset - 1], recv_sem=recv.at[part, phase, offset - 1],
            device_id=device(moved(axis, offset), core))

    def cross(part, index, full, place, side):
        view = region(part, full, place, side)
        return pltpu.make_async_remote_copy(
            src_ref=view, dst_ref=view,
            send_sem=across_send.at[part, index], recv_sem=across_recv.at[part, index],
            device_id=device(me, 1 - core))

    for part in range(parts):
        for offset in (1, 3, 2):
            hop(part, 0, offset, me).start()
        cross(part, 0, (), me, core).start()
    for index in range(1, 8):
        q_copy(index, side, me["x"]).start()
    for phase in range(3):
        for offset in (1, 3, 2):
            for part in range(parts):
                axis = orders[part][phase]
                source = moved(axis, 4 - offset)
                hop(part, phase, offset, source).wait_recv()
                cross(part, 3 * phase + offset, orders[part][:phase], source, core).start()
        if phase < 2:
            for part in range(parts):
                for offset in (1, 3, 2):
                    hop(part, phase + 1, offset, me).start()
    for part in range(parts):
        cross(part, 0, (), me, 1 - core).wait_recv()
        cross(part, 0, (), me, core).wait_send()
        for phase in range(3):
            for offset in (1, 3, 2):
                source = moved(orders[part][phase], 4 - offset)
                cross(part, 3 * phase + offset, orders[part][:phase], source, 1 - core).wait_recv()
                cross(part, 3 * phase + offset, orders[part][:phase], source, core).wait_send()
                hop(part, phase, offset, me).wait_send()
    q_own.wait()
    for index in range(1, 8):
        sender = (me["x"] + 4 - index % 4) % 4
        q_copy(index, side if index < 4 else 1 - side, sender).wait_recv()
        q_copy(index, side, me["x"]).wait_send()


def gather_everywhere(piece, q_rows):
    rows, width = piece.shape
    anywhere = pl.BlockSpec(memory_space=pl.ANY)
    return pl.pallas_call(
        gather_kernel,
        out_shape=(
            jax.ShapeDtypeStruct((4, 4, 2, 4, rows, width), bf16),
            jax.ShapeDtypeStruct((2, 4, q_rows.shape[0] // 2, q_rows.shape[1]), bf16),
        ),
        in_specs=[anywhere, anywhere],
        out_specs=(anywhere, anywhere),
        scratch_shapes=[
            pltpu.SemaphoreType.DMA,
            pltpu.SemaphoreType.DMA((3, 3, 3)),
            pltpu.SemaphoreType.DMA((3, 3, 3)),
            pltpu.SemaphoreType.DMA((3, 10)),
            pltpu.SemaphoreType.DMA((3, 10)),
            pltpu.SemaphoreType.DMA((8,)),
            pltpu.SemaphoreType.DMA((8,)),
        ],
        compiler_params=pltpu.CompilerParams(collective_id=0, has_side_effects=True),
        cost_estimate=pl.CostEstimate(flops=10**9, transcendentals=0, bytes_accessed=10**7),
    )(piece, q_rows)


def attention_kernel(idx_ref, q_ref, kv_ref, wk_ref, wv_ref, out_ref, top, acc, *, heads, rows, coef):
    step = pl.program_id(0)
    low, last, odd_low = idx_ref[0], idx_ref[1], idx_ref[2]

    @pl.when(step == 0)
    def _():
        top[...] = jnp.full(top.shape, LOW, f32)
        acc[...] = jnp.zeros(acc.shape, f32)

    wide_cols = q_ref.shape[2]
    half_cols = wide_cols // 2

    def block(both, masked):
        span = slice(0, wide_cols) if both else slice(half_cols, wide_cols)
        piece = kv_ref[0]
        count = piece.shape[0]
        latent = piece.shape[2]
        normed = piece[:, :rows, :].reshape(count * rows, latent)
        strips = []
        lane = lax.broadcasted_iota(jnp.int32, (piece.shape[1] - rows, 128), 1)
        inside = (lane >= NOPE) & (lane < NOPE + ROPE)
        for t in range(count):
            for c in range(2):
                tail = piece[t, rows:, c * 128 : (c + 1) * 128].astype(f32)
                for j in range(4):
                    shift = (NOPE - ROPE * j) % 128
                    strip = pltpu.roll(tail, shift, 1) if shift else tail
                    strips.append(jnp.where(inside, strip, 0.0))
        turned = jnp.concatenate(strips, axis=0)
        keys = jnp.dot(normed, wk_ref[...], preferred_element_type=f32)
        vals = lax.dot_general(
            wv_ref[...], normed, (((1,), (1,)), ((), ())), preferred_element_type=f32
        ).astype(bf16)
        ones = jnp.ones((16, count * rows), bf16)
        for h in range(heads):
            key_rows = (keys[:, h * 128 : (h + 1) * 128] + turned).astype(bf16)
            s = jnp.dot(key_rows, q_ref[h, :, span], preferred_element_type=f32)
            if masked:
                key_seg = lax.broadcasted_iota(jnp.int32, s.shape, 0) // SEG
                col = lax.broadcasted_iota(jnp.int32, s.shape, 1)
                query_seg = 2 * ((col % half_cols) // SEG)
                if both:
                    query_seg = jnp.where(col < half_cols, query_seg + odd_low, 2 * count)
                else:
                    query_seg = query_seg + 1 - odd_low
                s = jnp.where(key_seg <= query_seg, s, LOW)
            old = top[h, :, span]
            new = jnp.maximum(old, jnp.max(s, axis=0, keepdims=True))
            p = jnp.exp2((s - new) * coef).astype(bf16)
            factor = jnp.exp2((old - new) * coef)
            wide = jnp.concatenate([vals[h * VD : (h + 1) * VD], ones], axis=0)
            acc[h, :, span] = acc[h, :, span] * factor + jnp.dot(
                wide, p, preferred_element_type=f32
            )
            top[h, :, span] = new

    @pl.when(step < low)
    def _():
        block(True, False)

    @pl.when(step == low)
    def _():
        block(True, True)

    @pl.when((step > low) & (step < last))
    def _():
        block(False, False)

    @pl.when(step == last)
    def _():
        block(False, True)
        for h in range(heads):
            a = acc[h]
            out_ref[h * VD : (h + 1) * VD, :] = (a[:VD] / a[VD : VD + 1]).astype(bf16)


def attend(group, q_cat, kv, wk_wide, wv_turned):
    heads, _, queries = q_cat.shape
    blocks, count, piece_rows, latent = kv.shape
    rows = queries // count
    coef = ((NOPE + ROPE) ** -0.5) * math.log2(math.e)
    return pl.pallas_call(
        functools.partial(attention_kernel, heads=heads, rows=rows, coef=coef),
        out_shape=jax.ShapeDtypeStruct((heads * VD, queries), bf16),
        grid_spec=pltpu.PrefetchScalarGridSpec(
            num_scalar_prefetch=1,
            grid=(blocks,),
            in_specs=[
                pl.BlockSpec(q_cat.shape, lambda i, n: (0, 0, 0)),
                pl.BlockSpec(
                    (1, count, piece_rows, latent), lambda i, n: (jnp.minimum(i, n[1]), 0, 0, 0)
                ),
                pl.BlockSpec(wk_wide.shape, lambda i, n: (0, 0)),
                pl.BlockSpec(wv_turned.shape, lambda i, n: (0, 0)),
            ],
            out_specs=pl.BlockSpec((heads * VD, queries), lambda i, n: (0, 0)),
            scratch_shapes=[
                pltpu.VMEM((heads, 1, queries), f32),
                pltpu.VMEM((heads, VD + 16, queries), f32),
            ],
        ),
        compiler_params=pltpu.CompilerParams(
            dimension_semantics=("arbitrary",), vmem_limit_bytes=60 << 20
        ),
        cost_estimate=pl.CostEstimate(
            flops=3 * heads * 10**9, transcendentals=8 * heads * 10**6, bytes_accessed=10**7
        ),
    )(group, q_cat, kv, wk_wide, wv_turned)


def expert_kernel(x_hbm, w0, w1, w2, w3, out_ref, x_ref, w_ref, acc, sems, *, width):
    copies = [pltpu.make_async_copy(x_hbm, x_ref, sems.at[4])]
    for k, w in enumerate((w0, w1, w2, w3)):
        copies.append(pltpu.make_async_copy(w, w_ref.at[k], sems.at[k]))
    for copy in copies:
        copy.start()
    copies[0].wait()
    rows, feats = x_ref.shape
    tile = 256
    for k in range(4):
        copies[k + 1].wait()

        def body(r, carry):
            span = pl.ds(pl.multiple_of(r * tile, tile), tile)
            x = x_ref[span, :]
            gate = jnp.dot(x, w_ref[k, :feats, :], preferred_element_type=f32)
            up = jnp.dot(x, w_ref[k, feats : 2 * feats, :], preferred_element_type=f32)
            hidden = (gate / (1.0 + jnp.exp(-gate)) * up).astype(bf16)
            for j in range(feats // width):
                down = w_ref[k, 2 * feats + j * width : 2 * feats + (j + 1) * width, :]
                y = jnp.dot(hidden, down, preferred_element_type=f32).astype(bf16).astype(f32)
                cols = slice(j * width, (j + 1) * width)
                if k == 0:
                    acc[span, cols] = y
                elif k < 3:
                    acc[span, cols] = acc[span, cols] + y
                else:
                    out_ref[span, cols] = (acc[span, cols] + y).astype(bf16)
            return carry

        lax.fori_loop(0, rows // tile, body, 0)


def run_expert(rows_in, weights):
    rows, feats = rows_in.shape
    width = weights[0].shape[1]
    anywhere = pl.BlockSpec(memory_space=pl.ANY)
    return pl.pallas_call(
        functools.partial(expert_kernel, width=width),
        out_shape=jax.ShapeDtypeStruct((rows, feats), bf16),
        in_specs=[anywhere] * 5,
        out_specs=pl.BlockSpec(memory_space=pltpu.VMEM),
        scratch_shapes=[
            pltpu.VMEM((rows, feats), bf16),
            pltpu.VMEM((4,) + weights[0].shape, bf16),
            pltpu.VMEM((rows, feats), f32),
            pltpu.SemaphoreType.DMA((5,)),
        ],
        compiler_params=pltpu.CompilerParams(vmem_limit_bytes=40 << 20),
        cost_estimate=pl.CostEstimate(flops=10**10, transcendentals=10**6, bytes_accessed=2 * 10**7),
    )(rows_in, *weights)


def placed(z, y, core, x):
    return (z * 8 + y * 2 + core) * TP + x


chips = [(z, y, x) for z in range(4) for y in range(4) for x in range(4)]
across_pairs = [
    (placed(z, y, x // 2, x), placed(z, y, 1 - x // 2, x)) for z, y, x in chips
] + [(placed(z, y, 1 - x // 2, x), placed(z, y, 1 - x // 2, 3 - x)) for z, y, x in chips]
near_pairs = [(placed(z, y, x // 2, x), placed(z, y, x // 2, x ^ 1)) for z, y, x in chips]
over_pairs = [(placed(z, y, x // 2, x), placed(z, y, 1 - x // 2, x)) for z, y, x in chips]
row_groups = [
    [placed(z, y, core, x) for z in range(4) for y in range(4) for x in xs]
    for core in range(2)
    for xs in ((0, 3), (1, 2))
]
mix_groups = [[g * TP + x for g in (low, EP - 1 - low) for x in range(TP)] for low in range(EP // 2)]
EVERY = ("ep", "tp")


def on_device(
    q_latent,
    kv_latent,
    rope_key,
    q_gain,
    kv_gain,
    w_query,
    w_query_rot,
    w_key,
    w_value,
    w_mix_out,
    expert_input,
    ffn_gain,
    expert_ids,
    route_weights,
    w_gate_exp,
    w_up_exp,
    w_down_exp,
):
    tok_rows = q_latent.shape[0]
    group = lax.axis_index("ep")
    place = lax.axis_index("tp")
    group_rows = TP * tok_rows
    heads_here = w_key.shape[1] // NOPE
    latent_width = kv_latent.shape[1]

    block_width = w_gate_exp.shape[2]
    own = jnp.concatenate(
        [w_gate_exp[0], w_up_exp[0]]
        + [w_down_exp[0][:, j * block_width : (j + 1) * block_width] for j in range(D // block_width)],
        axis=0,
    )
    first = lax.ppermute(own, EVERY, across_pairs)
    near = lax.ppermute(own, EVERY, near_pairs)

    slot_count = 3 * tok_rows * TOPK // (2 * EP)
    normed = rms_scale(expert_input, ffn_gain).astype(bf16)
    routed = expert_ids.reshape(-1)
    onehot = (routed[:, None] == jnp.arange(EP, dtype=jnp.int32)[None, :]).astype(jnp.int32)
    slot_number = jnp.sum((jnp.cumsum(onehot, axis=0) - 1) * onehot, axis=-1)
    slot_place = (routed * slot_count + slot_number).reshape(tok_rows, TOPK)
    slot_line = jnp.arange(EP * slot_count, dtype=jnp.int32)
    picks = [slot_place[:, rank][:, None] == slot_line[None, :] for rank in range(TOPK)]
    dispatch = picks[0]
    for rank in range(1, TOPK):
        dispatch = dispatch | picks[rank]
    outgoing = lax.dot_general(
        dispatch.astype(bf16), normed, (((0,), (0,)), ((), ())), preferred_element_type=f32
    ).astype(bf16)
    arrived = lax.all_to_all(
        outgoing.reshape(EP, slot_count, D),
        EVERY,
        split_axis=0,
        concat_axis=0,
        tiled=True,
        axis_index_groups=row_groups,
    )

    token_start = group * group_rows + place * tok_rows
    cosine, sine_table = tables(token_start + jnp.arange(tok_rows, dtype=jnp.int32))
    kv_normed = rms_scale(kv_latent, kv_gain).astype(bf16)
    k_turned = rotate_pairs(rope_key.astype(f32), cosine, sine_table).astype(bf16)
    tail = k_turned.reshape(2, 4, tok_rows // 8, ROPE).transpose(2, 0, 1, 3).reshape(-1, latent_width)
    piece = jnp.concatenate([kv_normed, tail], axis=0)
    q_normed = rms_scale(q_latent, q_gain).astype(bf16)
    piece, q_normed, outgoing = lax.optimization_barrier((piece, q_normed, outgoing))
    kv, q_rows = gather_everywhere(piece, q_normed)
    first, near, kv = lax.optimization_barrier((first, near, kv))
    far = lax.ppermute(first, EVERY, near_pairs)
    near_over = lax.ppermute(near, EVERY, over_pairs)
    first_over = lax.ppermute(first, EVERY, over_pairs)
    kv = kv.reshape(EP, TP, -1, latent_width)

    q_rows = q_rows.reshape(group_rows, -1)
    high_side = (group >= EP // 2).astype(jnp.int32)
    low = jnp.minimum(group, EP - 1 - group).astype(jnp.int32)
    line = jnp.arange(group_rows, dtype=jnp.int32)
    part = line // (group_rows // 2)
    within = line % (group_rows // 2)
    position = (
        jnp.where(part == 0, low, EP - 1 - low) * group_rows
        + within // SEG * tok_rows
        + jnp.where(part == high_side, 0, SEG)
        + within % SEG
    )
    cosine, sine_table = tables(position)
    cosine, sine_table = cosine.T[None], sine_table.T[None]
    flat = (((0,), (1,)), ((), ()))
    plain = lax.dot_general(w_query, q_rows, flat, preferred_element_type=f32).astype(bf16)
    turned = lax.dot_general(w_query_rot, q_rows, flat, preferred_element_type=f32).reshape(
        heads_here, ROPE, group_rows
    )
    one, two = turned[:, : ROPE // 2], turned[:, ROPE // 2 :]
    q_cat = jnp.concatenate(
        [
            plain.reshape(heads_here, NOPE, group_rows),
            (one * cosine - two * sine_table).astype(bf16),
            (one * sine_table + two * cosine).astype(bf16),
            jnp.zeros((heads_here, 128 - NOPE - ROPE, group_rows), bf16),
        ],
        axis=1,
    )
    wk_wide = jnp.pad(
        w_key.reshape(latent_width, heads_here, NOPE), ((0, 0), (0, 0), (0, 128 - NOPE))
    ).reshape(latent_width, heads_here * 128)
    wv_turned = w_value.T
    bounds = jnp.stack([low, EP - 1 - low, high_side])
    half_heads = heads_here // 2
    attended = []

    def attend_heads(n, queries):
        return attend(
            bounds,
            queries,
            kv,
            wk_wide[:, n * half_heads * 128 : (n + 1) * half_heads * 128],
            wv_turned[n * half_heads * VD : (n + 1) * half_heads * VD],
        )

    attended.append(attend_heads(0, q_cat[:half_heads]))

    chosen = arrived.reshape(EP * slot_count, D)
    chosen, far, attended[0] = lax.optimization_barrier((chosen, far, attended[0]))
    far_over = lax.ppermute(far, EVERY, over_pairs)
    home = group % 2 == place // 2
    results = lax.cond(
        home,
        lambda: run_expert(chosen, (own, first, near, far)),
        lambda: run_expert(chosen, (first, first_over, near_over, far_over)),
    )
    second_queries = q_cat[half_heads:]
    results, second_queries = lax.optimization_barrier((results, second_queries))
    results = lax.all_to_all(
        results.reshape(EP, slot_count, D),
        EVERY,
        split_axis=0,
        concat_axis=0,
        tiled=True,
        axis_index_groups=row_groups,
    ).reshape(EP * slot_count, D)
    attended.append(attend_heads(1, second_queries))
    attention = jnp.concatenate(attended, axis=0)

    partial_mix = lax.dot_general(
        attention, w_mix_out, (((0,), (0,)), ((), ())), preferred_element_type=f32
    ).astype(bf16)
    partial_mix, results = lax.optimization_barrier((partial_mix, results))
    mix_blocks = lax.all_to_all(
        partial_mix.reshape(2 * TP, SEG, D),
        EVERY,
        split_axis=0,
        concat_axis=0,
        tiled=True,
        axis_index_groups=mix_groups,
    ).astype(f32)
    low_sum = jnp.sum(mix_blocks[:TP], axis=0)
    high_sum = jnp.sum(mix_blocks[TP:], axis=0)
    mixer_out = jnp.concatenate(
        [
            jnp.where(high_side == 0, low_sum, high_sum),
            jnp.where(high_side == 0, high_sum, low_sum),
        ],
        axis=0,
    ).astype(bf16)

    combined = jnp.zeros((tok_rows, D), f32)
    for rank in range(TOPK):
        fetched = jnp.dot(picks[rank].astype(bf16), results, preferred_element_type=f32)
        combined = combined + route_weights[:, rank : rank + 1] * fetched
    return (mixer_out, combined.astype(bf16))


def solution(mesh):
    return jax.shard_map(
        on_device,
        mesh=mesh,
        in_specs=(
            P(("ep", "tp"), None),
            P(("ep", "tp"), None),
            P(("ep", "tp"), None),
            P(),
            P(),
            P(None, "tp"),
            P(None, "tp"),
            P(None, "tp"),
            P(None, "tp"),
            P("tp", None),
            P(("ep", "tp"), None),
            P(),
            P(("ep", "tp"), None),
            P(("ep", "tp"), None),
            P("ep", None, "tp"),
            P("ep", None, "tp"),
            P("ep", "tp", None),
        ),
        out_specs=(P(("ep", "tp"), None), P(("ep", "tp"), None)),
        check_vma=False,
    )
```
